512 devices in a mesh: fs: 16 (over y, x), tp: 32 (over z, core).
Axes of the slice: x: 4, y: 4, z: 16, core: 2. Of those that a mesh axis runs over, the one named last changes fastest.
Arguments:
- saved_query_latent: bfloat16 [16384, 1536], P('fs', 'tp'), may hold values from -6 to 6
- saved_key_value_latent: bfloat16 [16384, 1024], P('fs', 'tp'), may hold values from -6 to 6
- query_cot: bfloat16 [16384, 6144], P('fs', 'tp'), may hold values from -0.046875 to 0.046875
- kv_cot: bfloat16 [16384, 8192], P('fs', 'tp'), may hold values from -0.046875 to 0.046875
- query_full_weight: float32 [1536, 6144], P('fs', 'tp'), may hold values from -0.6 to 0.6
- key_value_full_weight: float32 [1024, 8192], P('fs', 'tp'), may hold values from -0.6 to 0.6
- query_mom: float32 [1536, 6144], P('fs', 'tp'), may hold values from -50 to 50
- kv_mom: float32 [1024, 8192], P('fs', 'tp'), may hold values from -50 to 50
- query_left: bfloat16 [1536, 1536], P('fs'), may hold values from -1 to 1.5
- kv_left: bfloat16 [1024, 1024], P('fs'), may hold values from -1 to 1.5
- query_right: bfloat16 [32, 192, 192], P('tp'), may hold values from -1 to 1.5
- kv_right: bfloat16 [32, 256, 256], P('tp'), may hold values from -1 to 1.5
Outputs:
- query_mom_new: float32 [1536, 6144], P('fs', 'tp')
- kv_mom_new: float32 [1024, 8192], P('fs', 'tp')
- query_update: float32 [1536, 6144], P('fs', 'tp')
- kv_update: float32 [1024, 8192], P('fs', 'tp')
- query_weight: float32 [1536, 6144], P('fs', 'tp')
- kv_weight: float32 [1024, 8192], P('fs', 'tp')
- query_copy: bfloat16 [1536, 6144], P(None, 'tp')
- kv_copy: bfloat16 [1024, 8192], P(None, 'tp')
The draws below stay inside these ranges and needn't reach their ends.
All inputs are finite; a program needn't handle non-finite values.
Results may differ from the reference program's by a relative error of at most 0.0055.
Values may be sent and summed in bfloat16 or wider, within the bound.
A program may use at most 64 MiB of HBM per device.

```python
import jax
import jax.numpy as jnp

QUERY_RANK = 1536
KEY_VALUE_RANK = 1024
HEAD_COUNT = 32
QUERY_KEY_WIDTH = 192
KEY_VALUE_WIDTH = 256
TOKEN_COUNT = 16384


def increasing_order(key, rows, cols):
    base = jax.random.truncated_normal(key, -5.0, 5.0, (rows, cols), jnp.float32)
    row_scale = 10.0 ** (jnp.arange(rows, dtype=jnp.float32) / max(rows - 1, 1))
    col_scale = 10.0 ** (jnp.arange(cols, dtype=jnp.float32) / max(cols - 1, 1))
    return 0.1 * base * row_scale[:, None] * col_scale[None, :]


def positive_definite(key, order):
    first = jax.random.fold_in(key, 11)
    second = jax.random.fold_in(key, 12)
    off = jax.random.truncated_normal(first, -5.0, 5.0, (order, order), jnp.float32)
    off = (off + off.T) * (0.3 / (2.0 * order) ** 0.5)
    diag = jax.random.uniform(second, (order,), jnp.float32, 0.9, 1.5)
    eye = jnp.eye(order, dtype=jnp.float32)
    return off * (1.0 - eye) + eye * diag[None, :]


def draw_query_mom(key, part):
    return increasing_order(jax.random.fold_in(key, 1), QUERY_RANK, HEAD_COUNT * QUERY_KEY_WIDTH)


def draw_kv_mom(key, part):
    return increasing_order(jax.random.fold_in(key, 2), KEY_VALUE_RANK, HEAD_COUNT * KEY_VALUE_WIDTH)


def draw_query_left(key, part):
    return positive_definite(jax.random.fold_in(key, 3), QUERY_RANK).astype(jnp.bfloat16)


def draw_kv_left(key, part):
    return positive_definite(jax.random.fold_in(key, 4), KEY_VALUE_RANK).astype(jnp.bfloat16)


def draw_query_right(key, part):
    keys = jax.random.split(jax.random.fold_in(key, 5), HEAD_COUNT)
    return jax.vmap(lambda single: positive_definite(single, QUERY_KEY_WIDTH))(keys).astype(jnp.bfloat16)


def draw_kv_right(key, part):
    keys = jax.random.split(jax.random.fold_in(key, 6), HEAD_COUNT)
    return jax.vmap(lambda single: positive_definite(single, KEY_VALUE_WIDTH))(keys).astype(jnp.bfloat16)


def raised(result, key, source, target, blocks, factor):
    owner, partner = [(jnp.arange(result.shape[position]) // (result.shape[position] // blocks)).reshape([-1 if axis == position else 1 for axis in range(result.ndim)]) for position in (source, target)]
    chosen = jax.random.permutation(key, blocks)[partner]
    strong = (owner == chosen) | (owner == (partner + blocks // 2) % blocks)
    return jnp.where(strong, factor * result, result)


def levels(rng, extent, cuts, low, largest):
    def one(position, parts):
        steps = jax.random.uniform(jax.random.fold_in(jax.random.fold_in(rng, 6), position), (parts,), jnp.float32, low / len(cuts), largest / len(cuts))
        return jnp.repeat(jnp.exp(steps), extent[position] // parts).reshape((-1,) + (1,) * (len(extent) - position - 1))

    gain = one(*cuts[0])
    for cut in cuts[1:]:
        gain = gain * one(*cut)
    return gain


def centred(own_key, dims, spread, reach, shards=(), kind=jnp.bfloat16):
    result = spread * jax.random.normal(own_key, dims, jnp.float32)
    if shards:
        result = result * levels(own_key, dims, shards, -0.22, 0.18)
    return jnp.clip(result, -reach, reach).astype(kind)


def noise_with(stream_key, dims, deviation, most, pieces, heavy, kind=jnp.bfloat16):
    result = deviation * jax.random.normal(stream_key, dims, jnp.float32)
    if pieces:
        result = result * levels(stream_key, dims, pieces, -0.22, 0.18)
    return jnp.clip(raised(result, jax.random.fold_in(stream_key, 3), *heavy), -most, most).astype(kind)


def setup_inputs(seed: int = 0) -> dict:
    key_list = jax.random.split(jax.random.key(seed), 13)
    saved_query_latent = noise_with(key_list[0], (TOKEN_COUNT, QUERY_RANK), 1.0, 6.0, ((0, 16), (1, 32)), (0, 1, 32, 2.75))
    saved_key_value_latent = noise_with(key_list[1], (TOKEN_COUNT, KEY_VALUE_RANK), 1.0, 6.0, ((0, 16), (1, 32)), (0, 1, 32, 2.75))
    query_cot = centred(key_list[2], (TOKEN_COUNT, HEAD_COUNT * QUERY_KEY_WIDTH), (1.0 / TOKEN_COUNT ** 0.5), 0.046875, ((0, 16), (1, 32)))
    kv_cot = centred(key_list[3], (TOKEN_COUNT, HEAD_COUNT * KEY_VALUE_WIDTH), (1.0 / TOKEN_COUNT ** 0.5), 0.046875, ((0, 16), (1, 32)))
    query_full_weight = centred(key_list[4], (QUERY_RANK, HEAD_COUNT * QUERY_KEY_WIDTH), 0.1, 0.6, ((0, 16), (1, 32)), jnp.float32)
    key_value_full_weight = centred(key_list[5], (KEY_VALUE_RANK, HEAD_COUNT * KEY_VALUE_WIDTH), 0.1, 0.6, ((0, 16), (1, 32)), jnp.float32)
    query_mom = draw_query_mom(jax.random.fold_in(key_list[12], 71), 0)
    kv_mom = draw_kv_mom(jax.random.fold_in(key_list[12], 71), 0)
    query_left = draw_query_left(jax.random.fold_in(key_list[12], 71), 0)
    kv_left = draw_kv_left(jax.random.fold_in(key_list[12], 71), 0)
    query_right = draw_query_right(jax.random.fold_in(key_list[12], 71), 0)
    kv_right = draw_kv_right(jax.random.fold_in(key_list[12], 71), 0)
    return dict(saved_query_latent=saved_query_latent, saved_key_value_latent=saved_key_value_latent, query_cot=query_cot, kv_cot=kv_cot, query_full_weight=query_full_weight, key_value_full_weight=key_value_full_weight, query_mom=query_mom, kv_mom=kv_mom, query_left=query_left, kv_left=kv_left, query_right=query_right, kv_right=kv_right)


beta_mom = 0.9
learn_rate = 0.01

def precondition(moment, left, right, heads, width):
    half = moment.astype(jnp.bfloat16)
    pre_left = jnp.dot(left, half, preferred_element_type=jnp.float32)
    left_half = pre_left.astype(jnp.bfloat16).astype(jnp.float32)
    blocks = left_half.reshape(left_half.shape[0], heads, width)
    pre = jnp.einsum('rhd,hde->rhe', blocks, right.astype(jnp.float32))
    return pre.reshape(left_half.shape[0], heads * width)

def reference(saved_query_latent, saved_key_value_latent, query_cot, kv_cot, query_full_weight, key_value_full_weight, query_mom, kv_mom, query_left, kv_left, query_right, kv_right):
    query_grad = jnp.dot(saved_query_latent.astype(jnp.float32).T, query_cot.astype(jnp.float32))
    kv_grad = jnp.dot(saved_key_value_latent.astype(jnp.float32).T, kv_cot.astype(jnp.float32))
    query_mom_new = beta_mom * query_mom + query_grad
    kv_mom_new = beta_mom * kv_mom + kv_grad
    query_pre = precondition(query_mom_new, query_left, query_right, HEAD_COUNT, QUERY_KEY_WIDTH)
    kv_pre = precondition(kv_mom_new, kv_left, kv_right, HEAD_COUNT, KEY_VALUE_WIDTH)
    query_scale = jnp.sqrt(jnp.sum(query_mom_new * query_mom_new) / jnp.sum(query_pre * query_pre))
    kv_scale = jnp.sqrt(jnp.sum(kv_mom_new * kv_mom_new) / jnp.sum(kv_pre * kv_pre))
    query_update = query_scale * query_pre
    kv_update = kv_scale * kv_pre
    query_weight = query_full_weight - learn_rate * query_update
    kv_weight = key_value_full_weight - learn_rate * kv_update
    return (query_mom_new, kv_mom_new, query_update, kv_update, query_weight, kv_weight, query_weight.astype(jnp.bfloat16), kv_weight.astype(jnp.bfloat16))
```

```python
import functools

import jax
import jax.numpy as jnp
from jax import lax
from jax.experimental import pallas as pl
from jax.experimental.pallas import tpu as pltpu
from jax.sharding import Mesh
from jax.sharding import PartitionSpec as P

FS = ("fs_0", "fs_1")
TP = ("tp_0", "tp_1")

beta_mom = 0.9
learn_rate = 0.01

QR, KR = 96, 64
QW, KW = 192, 256
QF, KF = 48, 32
CF = QF + KF
MSG = 272
PIECES = ((0, 32), (32, 48), (48, 80))
N_Q_PIECES = 2
OWNER_DELAY = 3
F32, BF16 = jnp.float32, jnp.bfloat16


def dot(a, b):
    return jnp.dot(a, b, preferred_element_type=F32)


def dot_t(a, b):
    return lax.dot_general(a, b, (((1,), (1,)), ((), ())), preferred_element_type=F32)


def repeat_tail():
    row = lax.broadcasted_iota(jnp.int32, (QW, 256), 0)
    col = lax.broadcasted_iota(jnp.int32, (QW, 256), 1)
    return jnp.where(row == jnp.where(col < QW, col, col - 64), 1.0, 0.0).astype(BF16)


def pack(store, q, k):
    lane = lax.broadcasted_iota(jnp.int32, (QR // 2, 128), 1)
    store(0, q[:, :128].astype(BF16))
    tail = jnp.where(lane < 64, q[: QR // 2, 128:], q[QR // 2 :, 128:])
    store(96, tail.astype(BF16))
    store(144, k[:, :128].astype(BF16))
    store(208, k[:, 128:].astype(BF16))


def gather_kernel(
    ny, nx, nz,
    latq, latk, cotq, h_cotk, h_wq, h_wk, h_momq, h_momk, h_leftq, h_leftk, h_rightq, h_rightk,
    o_momq, o_momk, o_preq, o_prek, o_pre, o_w, o_sums,
    lat, cote, cotk, wq, wk, momq, momk, leftq, leftk, rightq, rightk,
    out_g, g, half, wfull, pfull, hq, hk, s_a, s_b,
    ring_recv, pair_recv, sems, load_sems,
):
    nf = ny * nx
    top = nz // 2
    y, x = lax.axis_index("fs_0"), lax.axis_index("fs_1")
    z, c = lax.axis_index("tp_0"), lax.axis_index("tp_1")
    fs = y * nx + x
    tp = z * 2 + c
    (ring_s, pair_s, g_s, g_r, h_s, h_r, w_s, w_r, p_s, p_r, a_s, a_r, b_s, b_r) = [
        sems.at[i] for i in range(14)
    ]

    def plane(d):
        t = lax.rem(fs + d, nf)
        return {"fs_0": t // nx, "fs_1": lax.rem(t, nx)}

    up, down = lax.rem(z + 1, nz), lax.rem(z + nz - 1, nz)

    loads = [
        pltpu.make_async_copy(src, dst, load_sems.at[i])
        for i, (src, dst) in enumerate(
            (
                (latq, lat.at[0, c, :QF]),
                (latk, lat.at[0, c, QF:]),
                (h_wq, wq),
                (h_wk, wk),
                (cotq, cote.at[:QW]),
                (cotq.at[128:], cote.at[QW:]),
                (h_cotk, cotk),
                (h_momq, momq),
                (h_momk, momk),
                (h_leftq, leftq),
                (h_leftk, leftk),
                (h_rightq, rightq),
                (h_rightk, rightk),
            )
        )
    ]
    for load in loads:
        load.start()

    barrier = pltpu.get_barrier_semaphore()
    for d in ({"tp_0": up}, {"tp_0": down}, {"tp_1": 1 - c}):
        pl.semaphore_signal(barrier, inc=1, device_id=d)
    for d in range(1, nf):
        pl.semaphore_signal(barrier, inc=1, device_id=plane(d))

    select = repeat_tail()

    def into(buffer, index):
        def store(at, value):
            buffer[index, at : at + value.shape[0], :] = value

        return store

    for load in loads[:4]:
        load.wait()
    pack(into(wfull, fs), dot(wq[...].astype(BF16), select), wk[...])

    pl.semaphore_wait(barrier, 3 + nf - 1)

    def send(src, dst, s_sem, r_sem, to):
        pltpu.make_async_remote_copy(
            src, dst, s_sem, r_sem, device_id=to, device_id_type=pl.DeviceIdType.MESH
        ).start()

    def wait(ref, sem):
        pltpu.make_async_copy(ref, ref, sem).wait()

    def part(slot, piece):
        lo, hi = PIECES[piece]
        return lat.at[slot, c, lo:hi]

    def forward(slot, to_slot, piece, to_z):
        send(
            part(slot, piece), part(to_slot, piece), ring_s,
            ring_recv.at[to_slot, piece], {"tp_0": to_z},
        )

    def share(slot, piece):
        send(part(slot, piece), part(slot, piece), pair_s, pair_recv.at[slot], {"tp_1": 1 - c})

    for p in range(len(PIECES)):
        forward(0, 1, p, up)
        forward(0, 2, p, down)
    for p in range(len(PIECES)):
        share(0, p)

    for load in loads[4:]:
        load.wait()
    delta = lax.rem(fs - z + nz, nz)
    own_step = jnp.minimum(delta, nz - delta)

    def partial_gradient(slot):
        wait(lat.at[slot, 1 - c], pair_recv.at[slot])
        lq = jnp.concatenate([lat[slot, 0, :QF, :], lat[slot, 1, :QF, :]], axis=0)
        lk = jnp.concatenate([lat[slot, 0, QF:, :], lat[slot, 1, QF:, :]], axis=0)
        pack(into(out_g, slot), dot_t(lq, cote[...]), dot(lk, cotk[...]))
        dist = (slot + 1) // 2
        owner = lax.rem(z + jnp.where(lax.rem(slot, 2) == 1, nz - dist, dist), nz)

        @pl.when(owner != fs)
        def _():
            send(
                out_g.at[slot], g.at[fs], g_s, g_r,
                {"fs_0": owner // nx, "fs_1": lax.rem(owner, nx)},
            )

        @pl.when(owner == fs)
        def _():
            g[fs] = out_g[slot]

    def momentum():
        wait(g.at[: nf - 1], g_r)
        total = g[0].astype(F32)
        for i in range(1, nf):
            total += g[i].astype(F32)
        tail = total[96:144]
        tail = jnp.concatenate([tail, pltpu.roll(tail, 64, 1)], axis=0)
        o_momq[:, :128] = beta_mom * momq[:, :128] + total[:96]
        o_momq[:, 128:] = beta_mom * momq[:, 128:] + tail[:, :64]
        o_momk[:, :128] = beta_mom * momk[:, :128] + total[144:208]
        o_momk[:, 128:] = beta_mom * momk[:, 128:] + total[208:272]
        pack(into(half, fs), dot(o_momq[...].astype(BF16), select), o_momk[...])
        for d in range(1, nf):
            send(half.at[fs], half.at[fs], h_s, h_r, plane(d))

    def step(k, carry):
        for p in range(len(PIECES)):
            is_q = p < N_Q_PIECES
            a, b = 2 * k - 1, jnp.minimum(2 * k, nz - 1)
            last_a, last_b = (top, top - 1) if is_q else (top - 1, top)

            @pl.when(k <= last_a)
            def _():
                wait(part(a, p), ring_recv.at[a, p])

                @pl.when(k < last_a)
                def _():
                    forward(a, a + 2, p, up)

                share(a, p)

            @pl.when(k <= last_b)
            def _():
                wait(part(b, p), ring_recv.at[b, p])

                @pl.when(k < last_b)
                def _():
                    forward(b, jnp.minimum(b + 2, nz - 1), p, down)

                share(b, p)

        for d in (2 * k - 1, 2 * k):

            @pl.when(d < nf)
            def _():
                send(wfull.at[fs], wfull.at[fs], w_s, w_r, plane(d))

        @pl.when(k >= 2)
        def _():
            partial_gradient(2 * k - 3)

        @pl.when(k <= top)
        def _():
            partial_gradient(2 * k - 2)

        @pl.when(k == jnp.minimum(own_step + OWNER_DELAY, top + 1))
        def _():
            momentum()

        return carry

    lax.fori_loop(1, top + 2, step, 0)

    wait(half.at[: nf - 1], h_r)

    def spread(s, carry):
        tail = half[s, 96:144, :]
        rolled = pltpu.roll(tail.astype(F32), 64, 1).astype(BF16)
        hq[s, :, :128] = half[s, :96, :]
        hq[s, :48, 128:] = tail
        hq[s, 48:, 128:] = rolled
        hk[s, :, :128] = half[s, 144:208, :]
        hk[s, :, 128:] = half[s, 208:272, :]
        return carry

    lax.fori_loop(0, nf, spread, 0)
    left_q = dot(leftq[...], hq[...].reshape(nf * QR, 256))[:, :QW].astype(BF16)
    left_k = dot(leftk[...], hk[...].reshape(nf * KR, 256)).astype(BF16)
    right_q = dot(rightq[0], select).astype(BF16)
    pre_q = dot(left_q, right_q)
    pre_k = dot(left_k, rightk[0])
    pack(into(pfull, fs), pre_q, pre_k)
    o_preq[...] = pre_q[:, :QW]
    o_prek[...] = pre_k
    lane = lax.broadcasted_iota(jnp.int32, (1, 128), 1)
    sums = jnp.zeros((1, 128), F32)
    for i, v in enumerate((o_momq[...], o_momk[...], pre_q[:, :QW], pre_k)):
        sums = jnp.where(lane == i, jnp.sum(v * v), sums)
    s_a[fs] = sums
    for d in range(1, nf):
        send(s_a.at[fs], s_a.at[fs], a_s, a_r, plane(d))
    for d in range(1, nf):
        send(pfull.at[fs], pfull.at[fs], p_s, p_r, plane(d))
    wait(s_a.at[: nf - 1], a_r)
    total = s_a[0]
    for i in range(1, nf):
        total += s_a[i]
    s_b[tp] = total

    def column(d):
        t = lax.rem(tp + d, 2 * nz)
        return {"tp_0": t // 2, "tp_1": lax.rem(t, 2)}

    for d in range(1, 2 * nz):
        send(s_b.at[tp], s_b.at[tp], b_s, b_r, column(d))
    wait(wfull.at[: nf - 1], w_r)
    wait(pfull.at[: nf - 1], p_r)
    o_w[...] = wfull[...]
    o_pre[...] = pfull[...]
    wait(s_b.at[: 2 * nz - 1], b_r)
    total = s_b[0]
    for i in range(1, 2 * nz):
        total += s_b[i]
    o_sums[...] = total

    wait(lat.at[: nz - 1, 0], ring_s)
    wait(lat.at[:, 0], pair_s)
    wait(out_g.at[: nf - 1], g_s)
    wait(half.at[: nf - 1], h_s)
    wait(wfull.at[: nf - 1], w_s)
    wait(pfull.at[: nf - 1], p_s)
    wait(s_a.at[: nf - 1], a_s)
    wait(s_b.at[: 2 * nz - 1], b_s)


def finish_kernel(
    nf, sums, preq, prek, pre, w, wq, wk, momq, momk,
    o_momq, o_momk, o_updq, o_updk, o_wq, o_wk, o_cq, o_ck, cq,
):
    v = sums[...]
    lane = lax.broadcasted_iota(jnp.int32, (1, 128), 1)
    scales = jnp.sqrt(v / pltpu.roll(v, 126, 1))
    scale_q, scale_k = [
        jnp.sum(jnp.where(lane == i, scales, 0.0), axis=1, keepdims=True) for i in (0, 1)
    ]
    o_momq[...] = momq[...]
    o_momk[...] = momk[...]
    upd_q = scale_q * preq[...]
    upd_k = scale_k * prek[...]
    o_updq[...] = upd_q
    o_updk[...] = upd_k
    o_wq[...] = wq[...] - learn_rate * upd_q
    o_wk[...] = wk[...] - learn_rate * upd_k

    def body(s, carry):
        q = w[s, :144, :].astype(F32) - learn_rate * (scale_q * pre[s, :144, :].astype(F32))
        k = w[s, 144:, :].astype(F32) - learn_rate * (scale_k * pre[s, 144:, :].astype(F32))
        tail = q[96:]
        cq[s, :, :128] = q[:96].astype(BF16)
        cq[s, :48, 128:] = tail.astype(BF16)
        cq[s, 48:, 128:] = pltpu.roll(tail, 64, 1).astype(BF16)
        rows = pl.ds(pl.multiple_of(s * KR, KR), KR)
        o_ck[rows, :128] = k[:64].astype(BF16)
        o_ck[rows, 128:] = k[64:].astype(BF16)
        return carry

    lax.fori_loop(0, nf, body, 0)
    row = lax.broadcasted_iota(jnp.int32, (QW, 256), 0)
    col = lax.broadcasted_iota(jnp.int32, (QW, 256), 1)
    eye = jnp.where(row == col, 1.0, 0.0).astype(BF16)
    o_cq[...] = dot_t(eye, cq[...].reshape(nf * QR, 256)).astype(BF16)


def on_device(
    ny, nx, nz,
    saved_query_latent,
    saved_key_value_latent,
    query_cot,
    kv_cot,
    query_full_weight,
    key_value_full_weight,
    query_mom,
    kv_mom,
    query_left,
    kv_left,
    query_right,
    kv_right,
):
    nf = ny * nx
    tokens = query_cot.shape[0]
    vmem = pl.BlockSpec(memory_space=pltpu.VMEM)
    shape = jax.ShapeDtypeStruct
    own_q, own_k = shape((QR, QW), F32), shape((KR, KW), F32)
    packed = shape((nf, MSG, 128), BF16)
    mom_q, mom_k, pre_q, pre_k, pre, w, sums = pl.pallas_call(
        functools.partial(gather_kernel, ny, nx, nz),
        out_shape=(own_q, own_k, own_q, own_k, packed, packed, shape((1, 128), F32)),
        in_specs=[pl.BlockSpec(memory_space=pltpu.HBM)] * 12,
        out_specs=(vmem,) * 7,
        scratch_shapes=[
            pltpu.VMEM((nz, 2, CF, tokens), BF16),
            pltpu.VMEM((256, tokens), BF16),
            pltpu.VMEM((tokens, KW), BF16),
            pltpu.VMEM((QR, QW), F32),
            pltpu.VMEM((KR, KW), F32),
            pltpu.VMEM((QR, QW), F32),
            pltpu.VMEM((KR, KW), F32),
            pltpu.VMEM((QR, nf * QR), BF16),
            pltpu.VMEM((KR, nf * KR), BF16),
            pltpu.VMEM((1, QW, QW), BF16),
            pltpu.VMEM((1, KW, KW), BF16),
            pltpu.VMEM((nz, MSG, 128), BF16),
            pltpu.VMEM((nf, MSG, 128), BF16),
            pltpu.VMEM((nf, MSG, 128), BF16),
            pltpu.VMEM((nf, MSG, 128), BF16),
            pltpu.VMEM((nf, MSG, 128), BF16),
            pltpu.VMEM((nf, QR, 256), BF16),
            pltpu.VMEM((nf, KR, 256), BF16),
            pltpu.VMEM((nf, 1, 128), F32),
            pltpu.VMEM((2 * nz, 1, 128), F32),
            pltpu.SemaphoreType.DMA((nz, len(PIECES))),
            pltpu.SemaphoreType.DMA((nz,)),
            pltpu.SemaphoreType.DMA((14,)),
            pltpu.SemaphoreType.DMA((13,)),
        ],
        compiler_params=pltpu.CompilerParams(
            collective_id=0, has_side_effects=True
        ),
    )(
        saved_query_latent.T, saved_key_value_latent.T, query_cot.T, kv_cot,
        query_full_weight, key_value_full_weight, query_mom, kv_mom,
        query_left, kv_left, query_right, kv_right,
    )
    outs = pl.pallas_call(
        functools.partial(finish_kernel, nf),
        out_shape=(
            own_q, own_k, own_q, own_k, own_q, own_k,
            shape((QW, nf * QR), BF16), shape((nf * KR, KW), BF16),
        ),
        in_specs=[vmem] * 9,
        out_specs=(vmem,) * 8,
        scratch_shapes=[pltpu.VMEM((nf, QR, 256), BF16)],
        compiler_params=pltpu.CompilerParams(vmem_limit_bytes=32 * 2**20),
    )(sums, pre_q, pre_k, pre, w, query_full_weight, key_value_full_weight, mom_q, mom_k)
    return (*outs[:6], outs[6].T, outs[7])


def solution(mesh, dims=(4, 4, 16)):
    torus = Mesh(mesh.devices.reshape(*dims, 2), (*FS, *TP))
    placed = (P(FS, TP),) * 8 + (P(FS, None),) * 2 + (P(TP, None, None),) * 2
    return jax.shard_map(
        functools.partial(on_device, *dims),
        mesh=torus,
        in_specs=placed,
        out_specs=(P(FS, TP),) * 6 + (P(None, TP),) * 2,
        check_vma=False,
    )
```

```python
import functools

import jax
import jax.numpy as jnp
from jax import lax
from jax.experimental import pallas as pl
from jax.experimental.pallas import tpu as pltpu
from jax.sharding import Mesh
from jax.sharding import PartitionSpec as P

FS = ("fs_0", "fs_1")
TP = ("tp_0", "tp_1")

beta_mom = 0.9
learn_rate = 0.01

QR, KR = 96, 64
QW, KW = 192, 256
QF, KF = 48, 32
CF = QF + KF
QP, KP = 144, 128
PIECES = ((0, 32), (32, 48), (48, 80))
N_Q_PIECES = 2
DELAY = 2
F32, BF16 = jnp.float32, jnp.bfloat16


def dot(a, b):
    return jnp.dot(a, b, preferred_element_type=F32)


def dot_t(a, b):
    return lax.dot_general(a, b, (((1,), (1,)), ((), ())), preferred_element_type=F32)


def repeat_tail():
    row = lax.broadcasted_iota(jnp.int32, (QW, 256), 0)
    col = lax.broadcasted_iota(jnp.int32, (QW, 256), 1)
    return jnp.where(row == jnp.where(col < QW, col, col - 64), 1.0, 0.0).astype(BF16)


def pack_q(q):
    lane = lax.broadcasted_iota(jnp.int32, (QR // 2, 128), 1)
    tail = jnp.where(lane < 64, q[: QR // 2, 128:], q[QR // 2 :, 128:])
    return jnp.concatenate([q[:, :128], tail], axis=0).astype(BF16)


def pack_k(k):
    return jnp.concatenate([k[:, :128], k[:, 128:]], axis=0).astype(BF16)


def both(*conditions):
    return functools.reduce(jnp.logical_and, conditions)


def gather_kernel(
    ny, nx, nz,
    latq, latk, cotq, h_cotk, h_wq, h_wk, h_momq, h_momk, h_leftq, h_leftk, h_rightq, h_rightk,
    o_momq, o_momk, o_preq, o_prek, o_pq, o_pk, o_bq, o_bk, o_sums,
    lat, cote, cotk, wq, wk, momq, momk, leftq, leftk, rightq, rightk,
    outq, outk, rowq, rowk, midq, midk, ownq, ownk,
    halfq, halfk, wallq, wallk, pallq, pallk, hq, hk, s_a, s_b,
    ring_recv, pair_recv, row_recv, col_recv, cast_recv, sems, load_sems,
):
    nf = ny * nx
    top = nz // 2
    y, x = lax.axis_index("fs_0"), lax.axis_index("fs_1")
    z, c = lax.axis_index("tp_0"), lax.axis_index("tp_1")
    fs = y * nx + x
    tp = z * 2 + c
    ring_s, pair_s, g0q, g0k, g1q, g1k, r1q, r1k, a_s, a_r, b_s, b_r = [
        sems.at[i] for i in range(12)
    ]

    def row_peer(d):
        return {"fs_1": lax.rem(x + d, nx)}

    def col_peer(d):
        return {"fs_0": lax.rem(y + d, ny)}

    def plane(d):
        t = lax.rem(fs + d, nf)
        return {"fs_0": t // nx, "fs_1": lax.rem(t, nx)}

    up, down = lax.rem(z + 1, nz), lax.rem(z + nz - 1, nz)

    loads = [
        pltpu.make_async_copy(src, dst, load_sems.at[i])
        for i, (src, dst) in enumerate(
            (
                (latq, lat.at[0, c, :QF]),
                (latk, lat.at[0, c, QF:]),
                (h_wq, wq),
                (h_wk, wk),
                (cotq, cote.at[:QW]),
                (cotq.at[128:], cote.at[QW:]),
                (h_cotk, cotk),
                (h_momq, momq),
                (h_momk, momk),
                (h_leftq, leftq),
                (h_leftk, leftk),
                (h_rightq, rightq),
                (h_rightk, rightk),
            )
        )
    ]
    for load in loads:
        load.start()

    barrier = pltpu.get_barrier_semaphore()
    for d in ({"tp_0": up}, {"tp_0": down}, {"tp_1": 1 - c}):
        pl.semaphore_signal(barrier, inc=1, device_id=d)
    for d in range(1, nf):
        pl.semaphore_signal(barrier, inc=1, device_id=plane(d))

    select = repeat_tail()

    for load in loads[:4]:
        load.wait()
    wallq[fs] = pack_q(dot(wq[...].astype(BF16), select))
    wallk[fs] = pack_k(wk[...])

    pl.semaphore_wait(barrier, 3 + nf - 1)

    def send(src, dst, s_sem, r_sem, to):
        pltpu.make_async_remote_copy(
            src, dst, s_sem, r_sem, device_id=to, device_id_type=pl.DeviceIdType.MESH
        ).start()

    def wait(ref, sem):
        pltpu.make_async_copy(ref, ref, sem).wait()

    def part(slot, piece):
        lo, hi = PIECES[piece]
        return lat.at[slot, c, lo:hi]

    def forward(slot, to_slot, piece, to_z):
        send(
            part(slot, piece), part(to_slot, piece), ring_s,
            ring_recv.at[to_slot, piece], {"tp_0": to_z},
        )

    def share(slot, piece):
        send(part(slot, piece), part(slot, piece), pair_s, pair_recv.at[slot], {"tp_1": 1 - c})

    for p in range(len(PIECES)):
        forward(0, 1, p, up)
        forward(0, 2, p, down)
    for p in range(len(PIECES)):
        share(0, p)

    class Cast:
        def __init__(self, which, q, k):
            self.q, self.k = q, k
            self.which = which
            self.sq, self.sk, self.rq, self.rk = [cast_recv.at[which, i] for i in range(4)]

        def along_x(self, block, s_sem, r_sem):
            for d in range(1, nx):
                send(block, block, s_sem, r_sem, row_peer(d))

        def along_y(self, block, s_sem, r_sem):
            for d in range(1, ny):
                send(block, block, s_sem, r_sem, col_peer(d))

        def start(self):
            q, k = self.q.at[fs], self.k.at[fs]
            self.along_x(q, self.sq, row_recv.at[self.which, x])
            self.along_y(k, self.sk, col_recv.at[self.which, y])
            self.along_y(q, self.sq, self.rq)
            self.along_x(k, self.sk, self.rk)

        def pass_q(self, xs):
            block = self.q.at[y * nx + xs]
            wait(block, row_recv.at[self.which, xs])
            self.along_y(block, self.sq, self.rq)

        def pass_k(self, ys):
            block = self.k.at[ys * nx + x]
            wait(block, col_recv.at[self.which, ys])
            self.along_x(block, self.sk, self.rk)

        def finish(self):
            wait(self.q.at[: (ny - 1) * nx], self.rq)
            wait(self.k.at[: (nx - 1) * ny], self.rk)

        def drain(self):
            wait(self.q.at[: nf - 1], self.sq)
            wait(self.k.at[: nf - 1], self.sk)

    weights, halves, pres = Cast(0, wallq, wallk), Cast(1, halfq, halfk), Cast(2, pallq, pallk)
    weights.start()

    for load in loads[4:]:
        load.wait()
    delta = lax.rem(fs - z + nz, nz)
    own_step = jnp.minimum(delta, nz - delta)

    def partial_gradient(slot, s):
        wait(lat.at[slot, 1 - c], pair_recv.at[slot])
        lq = jnp.concatenate([lat[slot, 0, :QF, :], lat[slot, 1, :QF, :]], axis=0)
        lk = jnp.concatenate([lat[slot, 0, QF:, :], lat[slot, 1, QF:, :]], axis=0)
        outq[slot] = pack_q(dot_t(lq, cote[...]))
        outk[slot] = pack_k(dot(lk, cotk[...]))
        ys, xs = s // nx, lax.rem(s, nx)

        @pl.when(xs != x)
        def _():
            send(outq.at[slot], rowq.at[ys, x], g0q, pair_recv.at[nz + ys], {"fs_1": xs})

        @pl.when(xs == x)
        def _():
            rowq[ys, x] = outq[slot]

        @pl.when(ys != y)
        def _():
            send(outk.at[slot], rowk.at[xs, y], g0k, pair_recv.at[nz + ny + xs], {"fs_0": ys})

        @pl.when(ys == y)
        def _():
            rowk[xs, y] = outk[slot]

    def added(ref, index, n):
        total = ref[index, 0].astype(F32)
        for i in range(1, n):
            total += ref[index, i].astype(F32)
        return total

    def reduce_first(slot, s):
        ys, xs = s // nx, lax.rem(s, nx)

        @pl.when(xs == x)
        def _():
            wait(rowq.at[ys, : nx - 1], pair_recv.at[nz + ys])
            total = added(rowq, ys, nx).astype(BF16)

            @pl.when(ys != y)
            def _():
                midq[ys] = total
                send(midq.at[ys], ownq.at[0, y], g1q, r1q, {"fs_0": ys})

            @pl.when(ys == y)
            def _():
                ownq[0, y] = total

        @pl.when(ys == y)
        def _():
            wait(rowk.at[xs, : ny - 1], pair_recv.at[nz + ny + xs])
            total = added(rowk, xs, ny).astype(BF16)

            @pl.when(xs != x)
            def _():
                midk[xs] = total
                send(midk.at[xs], ownk.at[0, x], g1k, r1k, {"fs_1": xs})

            @pl.when(xs == x)
            def _():
                ownk[0, x] = total

    def momentum():
        wait(ownq.at[0, : ny - 1], r1q)
        wait(ownk.at[0, : nx - 1], r1k)
        q, k = added(ownq, 0, ny), added(ownk, 0, nx)
        tail = q[QR:]
        tail = jnp.concatenate([tail, pltpu.roll(tail, 64, 1)], axis=0)
        o_momq[:, :128] = beta_mom * momq[:, :128] + q[:QR]
        o_momq[:, 128:] = beta_mom * momq[:, 128:] + tail[:, :64]
        o_momk[:, :128] = beta_mom * momk[:, :128] + k[:KR]
        o_momk[:, 128:] = beta_mom * momk[:, 128:] + k[KR:]
        halfq[fs] = pack_q(dot(o_momq[...].astype(BF16), select))
        halfk[fs] = pack_k(o_momk[...])
        halves.start()

    def relay(slot, s):
        ys, xs = s // nx, lax.rem(s, nx)

        @pl.when(both(ys == y, xs != x))
        def _():
            halves.pass_q(xs)

        @pl.when(both(xs == x, ys != y))
        def _():
            halves.pass_k(ys)

    def per_slot(do, st):
        @pl.when(both(st >= 1, st <= top))
        def _():
            do(2 * st - 1, lax.rem(z + nz - st, nz))

        @pl.when(both(st >= 0, st < top))
        def _():
            do(2 * st, lax.rem(z + st, nz))

    def step(k, carry):
        for p in range(len(PIECES)):
            is_q = p < N_Q_PIECES
            a, b = 2 * k - 1, jnp.minimum(2 * k, nz - 1)
            last_a, last_b = (top, top - 1) if is_q else (top - 1, top)

            @pl.when(k <= last_a)
            def _():
                wait(part(a, p), ring_recv.at[a, p])

                @pl.when(k < last_a)
                def _():
                    forward(a, a + 2, p, up)

                share(a, p)

            @pl.when(k <= last_b)
            def _():
                wait(part(b, p), ring_recv.at[b, p])

                @pl.when(k < last_b)
                def _():
                    forward(b, jnp.minimum(b + 2, nz - 1), p, down)

                share(b, p)

        for i in range(1, max(nx, ny)):

            @pl.when(k == i + 2)
            def _():
                if i < nx:
                    weights.pass_q(lax.rem(x + i, nx))
                if i < ny:
                    weights.pass_k(lax.rem(y + i, ny))

        per_slot(partial_gradient, k - 1)
        per_slot(reduce_first, k - 1 - DELAY)

        @pl.when(k == own_step + 1 + 2 * DELAY)
        def _():
            momentum()

        per_slot(relay, k - 1 - 3 * DELAY)
        return carry

    lax.fori_loop(1, max(top + 2 + 3 * DELAY, max(nx, ny) + 2), step, 0)

    weights.finish()
    w_out = [
        pltpu.make_async_copy(wallq, o_bq, load_sems.at[0]),
        pltpu.make_async_copy(wallk, o_bk, load_sems.at[1]),
    ]
    for copy in w_out:
        copy.start()
    halves.finish()

    def spread(s, carry):
        tail = halfq[s, QR:, :]
        hq[s, :, :128] = halfq[s, :QR, :]
        hq[s, : QR // 2, 128:] = tail
        hq[s, QR // 2 :, 128:] = pltpu.roll(tail.astype(F32), 64, 1).astype(BF16)
        hk[s, :, :128] = halfk[s, :KR, :]
        hk[s, :, 128:] = halfk[s, KR:, :]
        return carry

    lax.fori_loop(0, nf, spread, 0)
    left_q = dot(leftq[...], hq[...].reshape(nf * QR, 256))[:, :QW].astype(BF16)
    left_k = dot(leftk[...], hk[...].reshape(nf * KR, 256)).astype(BF16)
    right_q = dot(rightq[0], select).astype(BF16)
    pre_q = dot(left_q, right_q)
    pre_k = dot(left_k, rightk[0])
    pallq[fs] = pack_q(pre_q)
    pallk[fs] = pack_k(pre_k)
    o_preq[...] = pre_q[:, :QW]
    o_prek[...] = pre_k
    lane = lax.broadcasted_iota(jnp.int32, (1, 128), 1)
    sums = jnp.zeros((1, 128), F32)
    for i, v in enumerate((o_momq[...], o_momk[...], pre_q[:, :QW], pre_k)):
        sums = jnp.where(lane == i, jnp.sum(v * v), sums)
    s_a[fs] = sums
    for d in range(1, nf):
        send(s_a.at[fs], s_a.at[fs], a_s, a_r, plane(d))
    pres.start()
    wait(s_a.at[: nf - 1], a_r)
    total = s_a[0]
    for i in range(1, nf):
        total += s_a[i]
    s_b[tp] = total

    def column(d):
        t = lax.rem(tp + d, 2 * nz)
        return {"tp_0": t // 2, "tp_1": lax.rem(t, 2)}

    for d in range(1, 2 * nz):
        send(s_b.at[tp], s_b.at[tp], b_s, b_r, column(d))
    for i in range(1, nx):
        pres.pass_q(lax.rem(x + i, nx))
    for i in range(1, ny):
        pres.pass_k(lax.rem(y + i, ny))
    pres.finish()
    p_out = [
        pltpu.make_async_copy(pallq, o_pq, load_sems.at[2]),
        pltpu.make_async_copy(pallk, o_pk, load_sems.at[3]),
    ]
    for copy in p_out:
        copy.start()
    wait(lat.at[: nz - 1, 0], ring_s)
    wait(lat.at[:, 0], pair_s)
    wait(outq.at[: nf - ny], g0q)
    wait(outk.at[: nf - nx], g0k)
    wait(midq.at[: ny - 1], g1q)
    wait(midk.at[: nx - 1], g1k)
    weights.drain()
    halves.drain()
    pres.drain()
    for copy in (*w_out, *p_out):
        copy.wait()
    wait(s_a.at[: nf - 1], a_s)
    wait(s_b.at[: 2 * nz - 1], b_s)
    wait(s_b.at[: 2 * nz - 1], b_r)
    total = s_b[0]
    for i in range(1, 2 * nz):
        total += s_b[i]
    o_sums[...] = total


def finish_kernel(
    nf, *refs,
):
    given, outs, held = refs[:11], refs[11:19], refs[19:30]
    cq, load_sems = refs[30:]
    o_momq, o_momk, o_updq, o_updk, o_wq, o_wk, o_cq, o_ck = outs
    loads = [
        pltpu.make_async_copy(src, dst, load_sems.at[i])
        for i, (src, dst) in enumerate(zip(given, held))
    ]
    for load in loads:
        load.start()
    row = lax.broadcasted_iota(jnp.int32, (QW, 256), 0)
    col = lax.broadcasted_iota(jnp.int32, (QW, 256), 1)
    eye = jnp.where(row == col, 1.0, 0.0).astype(BF16)
    for load in loads:
        load.wait()
    sums, preq, prek, pq, pk, bq, bk, wq, wk, momq, momk = held
    v = sums[...]
    lane = lax.broadcasted_iota(jnp.int32, (1, 128), 1)
    scales = jnp.sqrt(v / pltpu.roll(v, 126, 1))
    scale_q, scale_k = [
        jnp.sum(jnp.where(lane == i, scales, 0.0), axis=1, keepdims=True) for i in (0, 1)
    ]
    o_momq[...] = momq[...]
    o_momk[...] = momk[...]
    upd_q = scale_q * preq[...]
    upd_k = scale_k * prek[...]
    o_updq[...] = upd_q
    o_updk[...] = upd_k
    o_wq[...] = wq[...] - learn_rate * upd_q
    o_wk[...] = wk[...] - learn_rate * upd_k

    def body(s, carry):
        q = bq[s].astype(F32) - learn_rate * (scale_q * pq[s].astype(F32))
        k = bk[s].astype(F32) - learn_rate * (scale_k * pk[s].astype(F32))
        tail = q[QR:]
        cq[s, :, :128] = q[:QR].astype(BF16)
        cq[s, : QR // 2, 128:] = tail.astype(BF16)
        cq[s, QR // 2 :, 128:] = pltpu.roll(tail, 64, 1).astype(BF16)
        rows = pl.ds(pl.multiple_of(s * KR, KR), KR)
        o_ck[rows, :128] = k[:KR].astype(BF16)
        o_ck[rows, 128:] = k[KR:].astype(BF16)
        return carry

    lax.fori_loop(0, nf, body, 0)
    o_cq[...] = dot_t(eye, cq[...].reshape(nf * QR, 256)).astype(BF16)


def on_device(
    ny, nx, nz,
    saved_query_latent,
    saved_key_value_latent,
    query_cot,
    kv_cot,
    query_full_weight,
    key_value_full_weight,
    query_mom,
    kv_mom,
    query_left,
    kv_left,
    query_right,
    kv_right,
):
    nf = ny * nx
    tokens = query_cot.shape[0]
    vmem = pl.BlockSpec(memory_space=pltpu.VMEM)
    shape = jax.ShapeDtypeStruct
    own_q, own_k = shape((QR, QW), F32), shape((KR, KW), F32)
    all_q, all_k = shape((nf, QP, 128), BF16), shape((nf, KP, 128), BF16)
    row = shape((1, 128), F32)
    hbm = pl.BlockSpec(memory_space=pltpu.HBM)
    block_q, block_k = [lambda *n, r=r: pltpu.VMEM((*n, r, 128), BF16) for r in (QP, KP)]
    dma = pltpu.SemaphoreType.DMA
    mom_q, mom_k, pre_q, pre_k, p_q, p_k, b_q, b_k, sums = pl.pallas_call(
        functools.partial(gather_kernel, ny, nx, nz),
        out_shape=(own_q, own_k, own_q, own_k, all_q, all_k, all_q, all_k, row),
        in_specs=[hbm] * 12,
        out_specs=(vmem,) * 4 + (hbm,) * 4 + (vmem,),
        scratch_shapes=[
            pltpu.VMEM((nz, 2, CF, tokens), BF16),
            pltpu.VMEM((256, tokens), BF16),
            pltpu.VMEM((tokens, KW), BF16),
            pltpu.VMEM((QR, QW), F32),
            pltpu.VMEM((KR, KW), F32),
            pltpu.VMEM((QR, QW), F32),
            pltpu.VMEM((KR, KW), F32),
            pltpu.VMEM((QR, nf * QR), BF16),
            pltpu.VMEM((KR, nf * KR), BF16),
            pltpu.VMEM((1, QW, QW), BF16),
            pltpu.VMEM((1, KW, KW), BF16),
            block_q(nz),
            block_k(nz),
            block_q(ny, nx),
            block_k(nx, ny),
            block_q(ny),
            block_k(nx),
            block_q(1, ny),
            block_k(1, nx),
            *(block_q(nf), block_k(nf)) * 3,
            pltpu.VMEM((nf, QR, 256), BF16),
            pltpu.VMEM((nf, KR, 256), BF16),
            pltpu.VMEM((nf, 1, 128), F32),
            pltpu.VMEM((2 * nz, 1, 128), F32),
            dma((nz, len(PIECES))),
            dma((nz + ny + nx,)),
            dma((3, nx)),
            dma((3, ny)),
            dma((3, 4)),
            dma((12,)),
            dma((13,)),
        ],
        compiler_params=pltpu.CompilerParams(collective_id=0, has_side_effects=True),
    )(
        saved_query_latent.T, saved_key_value_latent.T, query_cot.T, kv_cot,
        query_full_weight, key_value_full_weight, query_mom, kv_mom,
        query_left, kv_left, query_right, kv_right,
    )
    given = (
        sums, pre_q, pre_k, p_q, p_k, b_q, b_k,
        query_full_weight, key_value_full_weight, mom_q, mom_k,
    )
    outs = pl.pallas_call(
        functools.partial(finish_kernel, nf),
        out_shape=(
            own_q, own_k, own_q, own_k, own_q, own_k,
            shape((QW, nf * QR), BF16), shape((nf * KR, KW), BF16),
        ),
        in_specs=[hbm] * 11,
        out_specs=(vmem,) * 8,
        scratch_shapes=[
            *(pltpu.VMEM(a.shape, a.dtype) for a in given),
            pltpu.VMEM((nf, QR, 256), BF16),
            dma((11,)),
        ],
    )(*given)
    return (*outs[:6], outs[6].T, outs[7])


def solution(mesh, dims=(4, 4, 16)):
    torus = Mesh(mesh.devices.reshape(*dims, 2), (*FS, *TP))
    placed = (P(FS, TP),) * 8 + (P(FS, None),) * 2 + (P(TP, None, None),) * 2
    return jax.shard_map(
        functools.partial(on_device, *dims),
        mesh=torus,
        in_specs=placed,
        out_specs=(P(FS, TP),) * 6 + (P(None, TP),) * 2,
        check_vma=False,
    )
```

```python
import functools

import jax
import jax.numpy as jnp
from jax import lax
from jax.experimental import pallas as pl
from jax.experimental.pallas import tpu as pltpu
from jax.sharding import Mesh
from jax.sharding import PartitionSpec as P

FS = ("fs_0", "fs_1")
TP = ("tp_0", "tp_1")

beta_mom = 0.9
learn_rate = 0.01

QR, KR = 96, 64
QW, KW = 192, 256
QF, KF = 48, 32
CF = QF + KF
QP, KP = 144, 128
PIECES = tuple((r, r + 16) for r in range(0, CF, 16))
N_Q_PIECES = 3
REDUCE, OWN = 2, 4
F32, BF16 = jnp.float32, jnp.bfloat16


def dot(a, b):
    return jnp.dot(a, b, preferred_element_type=F32)


def dot_t(a, b):
    return lax.dot_general(a, b, (((1,), (1,)), ((), ())), preferred_element_type=F32)


def repeat_tail():
    row = lax.broadcasted_iota(jnp.int32, (QW, 256), 0)
    col = lax.broadcasted_iota(jnp.int32, (QW, 256), 1)
    return jnp.where(row == jnp.where(col < QW, col, col - 64), 1.0, 0.0).astype(BF16)


def pack_q(q):
    lane = lax.broadcasted_iota(jnp.int32, (QR // 2, 128), 1)
    tail = jnp.where(lane < 64, q[: QR // 2, 128:], q[QR // 2 :, 128:])
    return jnp.concatenate([q[:, :128], tail], axis=0).astype(BF16)


def pack_k(k):
    return jnp.concatenate([k[:, :128], k[:, 128:]], axis=0).astype(BF16)


def farthest_first(n):
    return sorted(range(1, n), key=lambda d: -min(d, n - d))


def both(*conditions):
    return functools.reduce(jnp.logical_and, conditions)


def gather_kernel(
    ny, nx, nz,
    latq, latk, cotq, h_cotk, h_wq, h_wk, h_momq, h_momk, h_leftq, h_leftk, h_rightq, h_rightk,
    o_momq, o_momk, o_preq, o_prek, o_pq, o_pk, o_bq, o_bk, o_sums,
    lat, cote, cotk, wq, wk, momq, momk, leftq, leftk, rightq, rightk,
    outq, outk, rowq, rowk, colq, colk, newq,
    halfq, halfk, wallq, wallk, pallq, pallk, hq, hk, s_a, s_b,
    ring_recv, pair_recv, sum_recv, row_recv, col_recv, cast_recv, sems, load_sems,
):
    nf = ny * nx
    top = nz // 2
    y, x = lax.axis_index("fs_0"), lax.axis_index("fs_1")
    z, c = lax.axis_index("tp_0"), lax.axis_index("tp_1")
    fs = y * nx + x
    tp = z * 2 + c
    (ring_s, pair_s, g0q, g0k, g1q, g1k, a_s, a_r, b_s, b_r,
     h_sq, h_sk, h_rq, h_rk, m_sq, m_sk, m_rq, m_rk) = [sems.at[i] for i in range(18)]

    def row_peer(d):
        return {"fs_1": lax.rem(x + d, nx)}

    def col_peer(d):
        return {"fs_0": lax.rem(y + d, ny)}

    def plane(d):
        t = lax.rem(fs + d, nf)
        return {"fs_0": t // nx, "fs_1": lax.rem(t, nx)}

    up, down = lax.rem(z + 1, nz), lax.rem(z + nz - 1, nz)

    loads = [
        pltpu.make_async_copy(src, dst, load_sems.at[i])
        for i, (src, dst) in enumerate(
            (
                (latq, lat.at[0, c, :QF]),
                (latk, lat.at[0, c, QF:]),
                (h_wq, wq),
                (h_wk, wk),
                (cotq, cote.at[:QW]),
                (cotq.at[128:], cote.at[QW:]),
                (h_cotk, cotk),
                (h_momq, momq.at[y]),
                (h_momk, momk.at[x]),
                (h_leftq, leftq),
                (h_leftk, leftk),
                (h_rightq, rightq),
                (h_rightk, rightk),
            )
        )
    ]
    for load in loads:
        load.start()

    barrier = pltpu.get_barrier_semaphore()
    for d in ({"tp_0": up}, {"tp_0": down}, {"tp_1": 1 - c}):
        pl.semaphore_signal(barrier, inc=1, device_id=d)
    for d in range(1, nf):
        pl.semaphore_signal(barrier, inc=1, device_id=plane(d))

    select = repeat_tail()

    for load in loads[:4]:
        load.wait()
    wallq[fs] = pack_q(dot(wq[...].astype(BF16), select))
    wallk[fs] = pack_k(wk[...])

    pl.semaphore_wait(barrier, 3 + nf - 1)

    def send(src, dst, s_sem, r_sem, to):
        pltpu.make_async_remote_copy(
            src, dst, s_sem, r_sem, device_id=to, device_id_type=pl.DeviceIdType.MESH
        ).start()

    def wait(ref, sem):
        pltpu.make_async_copy(ref, ref, sem).wait()

    def part(slot, piece):
        lo, hi = PIECES[piece]
        return lat.at[slot, c, lo:hi]

    def forward(slot, to_slot, piece, to_z):
        send(
            part(slot, piece), part(to_slot, piece), ring_s,
            ring_recv.at[to_slot, piece], {"tp_0": to_z},
        )

    def share(slot, piece):
        send(part(slot, piece), part(slot, piece), pair_s, pair_recv.at[slot], {"tp_1": 1 - c})

    for p in range(len(PIECES)):
        forward(0, 1, p, up)
        forward(0, 2, p, down)
    for p in range(len(PIECES)):
        share(0, p)

    class Cast:
        def __init__(self, which, q, k):
            self.q, self.k = q, k
            self.which = which
            self.sq, self.sk, self.rq, self.rk = [cast_recv.at[which, i] for i in range(4)]

        def along_x(self, block, s_sem, r_sem):
            for d in range(1, nx):
                send(block, block, s_sem, r_sem, row_peer(d))

        def along_y(self, block, s_sem, r_sem):
            for d in range(1, ny):
                send(block, block, s_sem, r_sem, col_peer(d))

        def start(self):
            q, k = self.q.at[fs], self.k.at[fs]
            self.along_x(q, self.sq, row_recv.at[self.which, x])
            self.along_y(k, self.sk, col_recv.at[self.which, y])
            self.along_y(q, self.sq, self.rq)
            self.along_x(k, self.sk, self.rk)

        def pass_q(self, xs):
            block = self.q.at[y * nx + xs]
            wait(block, row_recv.at[self.which, xs])
            self.along_y(block, self.sq, self.rq)

        def pass_k(self, ys):
            block = self.k.at[ys * nx + x]
            wait(block, col_recv.at[self.which, ys])
            self.along_x(block, self.sk, self.rk)

        def finish(self):
            wait(self.q.at[: (ny - 1) * nx], self.rq)
            wait(self.k.at[: (nx - 1) * ny], self.rk)

        def drain(self):
            wait(self.q.at[: nf - 1], self.sq)
            wait(self.k.at[: nf - 1], self.sk)

    weights, pres = Cast(0, wallq, wallk), Cast(1, pallq, pallk)
    weights.start()

    for load in loads[4:]:
        load.wait()
    for d in range(1, ny):
        send(momq.at[y], momq.at[y], m_sq, m_rq, col_peer(d))
    for d in range(1, nx):
        send(momk.at[x], momk.at[x], m_sk, m_rk, row_peer(d))

    def partial_gradient(slot, s):
        wait(lat.at[slot, 1 - c], pair_recv.at[slot])
        lq = jnp.concatenate([lat[slot, 0, :QF, :], lat[slot, 1, :QF, :]], axis=0)
        lk = jnp.concatenate([lat[slot, 0, QF:, :], lat[slot, 1, QF:, :]], axis=0)
        outq[slot] = pack_q(dot_t(lq, cote[...]))
        outk[slot] = pack_k(dot(lk, cotk[...]))
        ys, xs = s // nx, lax.rem(s, nx)

        @pl.when(xs != x)
        def _():
            send(outq.at[slot], rowq.at[ys, x], g0q, pair_recv.at[nz + ys], {"fs_1": xs})

        @pl.when(xs == x)
        def _():
            rowq[ys, x] = outq[slot]

        @pl.when(ys != y)
        def _():
            send(outk.at[slot], rowk.at[xs, y], g0k, pair_recv.at[nz + ny + xs], {"fs_0": ys})

        @pl.when(ys == y)
        def _():
            rowk[xs, y] = outk[slot]

    def added(ref, index, n):
        total = ref[index, 0].astype(F32)
        for i in range(1, n):
            total += ref[index, i].astype(F32)
        return total

    def reduce_first(slot, s):
        ys, xs = s // nx, lax.rem(s, nx)

        @pl.when(xs == x)
        def _():
            wait(rowq.at[ys, : nx - 1], pair_recv.at[nz + ys])
            colq[ys, y] = added(rowq, ys, nx).astype(BF16)
            for d in range(1, ny):
                send(colq.at[ys, y], colq.at[ys, y], g1q, sum_recv.at[ys], col_peer(d))

        @pl.when(ys == y)
        def _():
            wait(rowk.at[xs, : ny - 1], pair_recv.at[nz + ny + xs])
            colk[xs, x] = added(rowk, xs, ny).astype(BF16)
            for d in range(1, nx):
                send(colk.at[xs, x], colk.at[xs, x], g1k, sum_recv.at[ny + xs], row_peer(d))

    def momentum(slot, s):
        ys, xs = s // nx, lax.rem(s, nx)

        @pl.when(xs == x)
        def _():
            wait(colq.at[ys, : ny - 1], sum_recv.at[ys])
            q = added(colq, ys, ny)
            tail = q[QR:]
            tail = jnp.concatenate([tail, pltpu.roll(tail, 64, 1)], axis=0)
            newq[:, :128] = beta_mom * momq[ys, :, :128] + q[:QR]
            newq[:, 128:] = beta_mom * momq[ys, :, 128:] + tail[:, :64]
            halfq[s] = pack_q(dot(newq[...].astype(BF16), select))
            for d in range(1, nx):
                send(halfq.at[s], halfq.at[s], h_sq, h_rq, row_peer(d))

            @pl.when(ys == y)
            def _():
                o_momq[...] = newq[...]

        @pl.when(ys == y)
        def _():
            wait(colk.at[xs, : nx - 1], sum_recv.at[ny + xs])
            k = added(colk, xs, nx)
            new_a = beta_mom * momk[xs, :, :128] + k[:KR]
            new_b = beta_mom * momk[xs, :, 128:] + k[KR:]
            halfk[s] = jnp.concatenate([new_a, new_b], axis=0).astype(BF16)
            for d in range(1, ny):
                send(halfk.at[s], halfk.at[s], h_sk, h_rk, col_peer(d))

            @pl.when(xs == x)
            def _():
                o_momk[:, :128] = new_a
                o_momk[:, 128:] = new_b

    def per_slot(st):
        def first(do):
            @pl.when(both(st >= 1, st <= top))
            def _():
                do(2 * st - 1, lax.rem(z + nz - st, nz))

        def second(do):
            @pl.when(both(st >= 0, st < top))
            def _():
                do(2 * st, lax.rem(z + st, nz))

        return first, second

    def ring(k, p):
        is_q = p < N_Q_PIECES
        a, b = 2 * k - 1, jnp.minimum(2 * k, nz - 1)
        last_a, last_b = (top, top - 1) if is_q else (top - 1, top)

        @pl.when(k <= last_a)
        def _():
            wait(part(a, p), ring_recv.at[a, p])

            @pl.when(k < last_a)
            def _():
                forward(a, a + 2, p, up)

            share(a, p)

        @pl.when(k <= last_b)
        def _():
            wait(part(b, p), ring_recv.at[b, p])

            @pl.when(k < last_b)
            def _():
                forward(b, jnp.minimum(b + 2, nz - 1), p, down)

            share(b, p)

    def step(k, carry):
        first, second = per_slot(k - 1)
        ring(k, 0)
        first(partial_gradient)
        ring(k, 1)
        for which in per_slot(k - 1 - REDUCE):
            which(reduce_first)
        ring(k, 2)
        second(partial_gradient)
        ring(k, 3)
        ring(k, 4)

        @pl.when(k == 3)
        def _():
            wait(momq.at[: ny - 1], m_rq)
            wait(momk.at[: nx - 1], m_rk)
            for i in range(1, nx):
                weights.pass_q(lax.rem(x + i, nx))
            for i in range(1, ny):
                weights.pass_k(lax.rem(y + i, ny))

        for which in per_slot(k - 1 - OWN):
            which(momentum)
        return carry

    lax.fori_loop(1, top + 2 + OWN, step, 0)

    weights.finish()
    w_out = [
        pltpu.make_async_copy(wallq, o_bq, load_sems.at[0]),
        pltpu.make_async_copy(wallk, o_bk, load_sems.at[1]),
    ]
    for copy in w_out:
        copy.start()
    wait(halfq.at[: (nx - 1) * ny], h_rq)
    wait(halfk.at[: (ny - 1) * nx], h_rk)

    def spread(s, carry):
        tail = halfq[s, QR:, :]
        hq[s, :, :128] = halfq[s, :QR, :]
        hq[s, : QR // 2, 128:] = tail
        hq[s, QR // 2 :, 128:] = pltpu.roll(tail.astype(F32), 64, 1).astype(BF16)
        hk[s, :, :128] = halfk[s, :KR, :]
        hk[s, :, 128:] = halfk[s, KR:, :]
        return carry

    lax.fori_loop(0, nf, spread, 0)
    left_q = dot(leftq[...], hq[...].reshape(nf * QR, 256))[:, :QW].astype(BF16)
    left_k = dot(leftk[...], hk[...].reshape(nf * KR, 256)).astype(BF16)
    right_q = dot(rightq[0], select).astype(BF16)
    pre_q = dot(left_q, right_q)
    pre_k = dot(left_k, rightk[0])
    pallq[fs] = pack_q(pre_q)
    pallk[fs] = pack_k(pre_k)
    o_preq[...] = pre_q[:, :QW]
    o_prek[...] = pre_k
    lane = lax.broadcasted_iota(jnp.int32, (1, 128), 1)
    sums = jnp.zeros((1, 128), F32)
    for i, v in enumerate((o_momq[...], o_momk[...], pre_q[:, :QW], pre_k)):
        sums = jnp.where(lane == i, jnp.sum(v * v), sums)
    s_a[fs] = sums
    for d in range(1, nf):
        send(s_a.at[fs], s_a.at[fs], a_s, a_r, plane(d))
    pres.start()
    wait(s_a.at[: nf - 1], a_r)
    total = s_a[0]
    for i in range(1, nf):
        total += s_a[i]
    s_b[tp] = total

    def column(d):
        t = lax.rem(tp + d, 2 * nz)
        return {"tp_0": t // 2, "tp_1": lax.rem(t, 2)}

    for d in farthest_first(2 * nz):
        send(s_b.at[tp], s_b.at[tp], b_s, b_r, column(d))
    for i in range(1, nx):
        pres.pass_q(lax.rem(x + i, nx))
    for i in range(1, ny):
        pres.pass_k(lax.rem(y + i, ny))
    pres.finish()
    p_out = [
        pltpu.make_async_copy(pallq, o_pq, load_sems.at[2]),
        pltpu.make_async_copy(pallk, o_pk, load_sems.at[3]),
    ]
    for copy in p_out:
        copy.start()
    wait(lat.at[: nz - 1, 0], ring_s)
    wait(lat.at[:, 0], pair_s)
    wait(outq.at[: nf - ny], g0q)
    wait(outk.at[: nf - nx], g0k)
    wait(outq.at[: ny * (ny - 1)], g1q)
    wait(outk.at[: nx * (nx - 1)], g1k)
    wait(outq.at[: ny * (nx - 1)], h_sq)
    wait(outk.at[: nx * (ny - 1)], h_sk)
    wait(momq.at[: ny - 1], m_sq)
    wait(momk.at[: nx - 1], m_sk)
    weights.drain()
    pres.drain()
    for copy in (*w_out, *p_out):
        copy.wait()
    wait(s_a.at[: nf - 1], a_s)
    wait(s_b.at[: 2 * nz - 1], b_s)
    wait(s_b.at[: 2 * nz - 1], b_r)
    total = s_b[0]
    for i in range(1, 2 * nz):
        total += s_b[i]
    o_sums[...] = total


def finish_kernel(
    nf, *refs,
):
    given, outs, held = refs[:11], refs[11:19], refs[19:30]
    cq, load_sems = refs[30:]
    o_momq, o_momk, o_updq, o_updk, o_wq, o_wk, o_cq, o_ck = outs
    loads = [
        pltpu.make_async_copy(src, dst, load_sems.at[i])
        for i, (src, dst) in enumerate(zip(given, held))
    ]
    for load in loads:
        load.start()
    row = lax.broadcasted_iota(jnp.int32, (QW, 256), 0)
    col = lax.broadcasted_iota(jnp.int32, (QW, 256), 1)
    eye = jnp.where(row == col, 1.0, 0.0).astype(BF16)
    for load in loads:
        load.wait()
    sums, preq, prek, pq, pk, bq, bk, wq, wk, momq, momk = held
    v = sums[...]
    lane = lax.broadcasted_iota(jnp.int32, (1, 128), 1)
    scales = jnp.sqrt(v / pltpu.roll(v, 126, 1))
    scale_q, scale_k = [
        jnp.sum(jnp.where(lane == i, scales, 0.0), axis=1, keepdims=True) for i in (0, 1)
    ]
    o_momq[...] = momq[...]
    o_momk[...] = momk[...]
    upd_q = scale_q * preq[...]
    upd_k = scale_k * prek[...]
    o_updq[...] = upd_q
    o_updk[...] = upd_k
    o_wq[...] = wq[...] - learn_rate * upd_q
    o_wk[...] = wk[...] - learn_rate * upd_k

    def body(s, carry):
        q = bq[s].astype(F32) - learn_rate * (scale_q * pq[s].astype(F32))
        k = bk[s].astype(F32) - learn_rate * (scale_k * pk[s].astype(F32))
        tail = q[QR:]
        cq[s, :, :128] = q[:QR].astype(BF16)
        cq[s, : QR // 2, 128:] = tail.astype(BF16)
        cq[s, QR // 2 :, 128:] = pltpu.roll(tail, 64, 1).astype(BF16)
        rows = pl.ds(pl.multiple_of(s * KR, KR), KR)
        o_ck[rows, :128] = k[:KR].astype(BF16)
        o_ck[rows, 128:] = k[KR:].astype(BF16)
        return carry

    lax.fori_loop(0, nf, body, 0)
    o_cq[...] = dot_t(eye, cq[...].reshape(nf * QR, 256)).astype(BF16)


def on_device(
    ny, nx, nz,
    saved_query_latent,
    saved_key_value_latent,
    query_cot,
    kv_cot,
    query_full_weight,
    key_value_full_weight,
    query_mom,
    kv_mom,
    query_left,
    kv_left,
    query_right,
    kv_right,
):
    nf = ny * nx
    tokens = query_cot.shape[0]
    vmem = pl.BlockSpec(memory_space=pltpu.VMEM)
    shape = jax.ShapeDtypeStruct
    own_q, own_k = shape((QR, QW), F32), shape((KR, KW), F32)
    all_q, all_k = shape((nf, QP, 128), BF16), shape((nf, KP, 128), BF16)
    row = shape((1, 128), F32)
    hbm = pl.BlockSpec(memory_space=pltpu.HBM)
    block_q, block_k = [lambda *n, r=r: pltpu.VMEM((*n, r, 128), BF16) for r in (QP, KP)]
    dma = pltpu.SemaphoreType.DMA
    mom_q, mom_k, pre_q, pre_k, p_q, p_k, b_q, b_k, sums = pl.pallas_call(
        functools.partial(gather_kernel, ny, nx, nz),
        out_shape=(own_q, own_k, own_q, own_k, all_q, all_k, all_q, all_k, row),
        in_specs=[hbm] * 12,
        out_specs=(vmem,) * 4 + (hbm,) * 4 + (vmem,),
        scratch_shapes=[
            pltpu.VMEM((nz, 2, CF, tokens), BF16),
            pltpu.VMEM((256, tokens), BF16),
            pltpu.VMEM((tokens, KW), BF16),
            pltpu.VMEM((QR, QW), F32),
            pltpu.VMEM((KR, KW), F32),
            pltpu.VMEM((ny, QR, QW), F32),
            pltpu.VMEM((nx, KR, KW), F32),
            pltpu.VMEM((QR, nf * QR), BF16),
            pltpu.VMEM((KR, nf * KR), BF16),
            pltpu.VMEM((1, QW, QW), BF16),
            pltpu.VMEM((1, KW, KW), BF16),
            block_q(nz),
            block_k(nz),
            block_q(ny, nx),
            block_k(nx, ny),
            block_q(ny, ny),
            block_k(nx, nx),
            pltpu.VMEM((QR, QW), F32),
            *(block_q(nf), block_k(nf)) * 3,
            pltpu.VMEM((nf, QR, 256), BF16),
            pltpu.VMEM((nf, KR, 256), BF16),
            pltpu.VMEM((nf, 1, 128), F32),
            pltpu.VMEM((2 * nz, 1, 128), F32),
            dma((nz, len(PIECES))),
            dma((nz + ny + nx,)),
            dma((ny + nx,)),
            dma((2, nx)),
            dma((2, ny)),
            dma((2, 4)),
            dma((18,)),
            dma((13,)),
        ],
        compiler_params=pltpu.CompilerParams(collective_id=0, has_side_effects=True),
    )(
        saved_query_latent.T, saved_key_value_latent.T, query_cot.T, kv_cot,
        query_full_weight, key_value_full_weight, query_mom, kv_mom,
        query_left, kv_left, query_right, kv_right,
    )
    given = (
        sums, pre_q, pre_k, p_q, p_k, b_q, b_k,
        query_full_weight, key_value_full_weight, mom_q, mom_k,
    )
    outs = pl.pallas_call(
        functools.partial(finish_kernel, nf),
        out_shape=(
            own_q, own_k, own_q, own_k, own_q, own_k,
            shape((QW, nf * QR), BF16), shape((nf * KR, KW), BF16),
        ),
        in_specs=[hbm] * 11,
        out_specs=(vmem,) * 8,
        scratch_shapes=[
            *(pltpu.VMEM(a.shape, a.dtype) for a in given),
            pltpu.VMEM((nf, QR, 256), BF16),
            dma((11,)),
        ],
    )(*given)
    return (*outs[:6], outs[6].T, outs[7])


def solution(mesh, dims=(4, 4, 16)):
    torus = Mesh(mesh.devices.reshape(*dims, 2), (*FS, *TP))
    placed = (P(FS, TP),) * 8 + (P(FS, None),) * 2 + (P(TP, None, None),) * 2
    return jax.shard_map(
        functools.partial(on_device, *dims),
        mesh=torus,
        in_specs=placed,
        out_specs=(P(FS, TP),) * 6 + (P(None, TP),) * 2,
        check_vma=False,
    )
```

```python
import functools

import jax
import jax.numpy as jnp
from jax import lax
from jax.experimental import pallas as pl
from jax.experimental.pallas import tpu as pltpu
from jax.sharding import Mesh
from jax.sharding import PartitionSpec as P

FS = ("fs_0", "fs_1")
TP = ("tp_0", "tp_1")

beta_mom = 0.9
learn_rate = 0.01

QR, KR = 96, 64
QW, KW = 192, 256
QF, KF = 48, 32
CF = QF + KF
QP, KP = 144, 128
PIECES = tuple((r, r + 16) for r in range(0, CF, 16))
N_Q_PIECES = 3
REDUCE, OWN = 2, 4
F32, BF16 = jnp.float32, jnp.bfloat16


def dot(a, b):
    return jnp.dot(a, b, preferred_element_type=F32)


def dot_t(a, b):
    return lax.dot_general(a, b, (((1,), (1,)), ((), ())), preferred_element_type=F32)


def repeat_tail():
    row = lax.broadcasted_iota(jnp.int32, (QW, 256), 0)
    col = lax.broadcasted_iota(jnp.int32, (QW, 256), 1)
    return jnp.where(row == jnp.where(col < QW, col, col - 64), 1.0, 0.0).astype(BF16)


def split_halves(n):
    col = lax.broadcasted_iota(jnp.int32, (1, n), 1)
    second = (col >= n // 2).astype(jnp.int32)
    col = col - second * (n // 2)
    block = sum((col >= i).astype(jnp.int32) for i in range(QR // 2, n // 2, QR // 2))
    source = col + (block + second) * (QR // 2)
    row = lax.broadcasted_iota(jnp.int32, (n, n), 0)
    return jnp.where(row == source, 1.0, 0.0).astype(BF16)


def pack_q(q):
    lane = lax.broadcasted_iota(jnp.int32, (QR // 2, 128), 1)
    tail = jnp.where(lane < 64, q[: QR // 2, 128:], q[QR // 2 :, 128:])
    return jnp.concatenate([q[:, :128], tail], axis=0).astype(BF16)


def pack_k(k):
    return jnp.concatenate([k[:, :128], k[:, 128:]], axis=0).astype(BF16)


def farthest_first(n):
    return sorted(range(1, n), key=lambda d: -min(d, n - d))


def both(*conditions):
    return functools.reduce(jnp.logical_and, conditions)


def gather_kernel(
    ny, nx, nz,
    latq, latk, cotq, h_cotk, h_wq, h_wk, h_momq, h_momk, h_leftq, h_leftk, h_rightq, h_rightk,
    to_momq, to_momk, to_preq, to_prek, to_pq, to_pk, to_bq, to_bk, o_sums,
    lat, cote, cotk, wq, wk, momq, momk, leftq, leftk, rightq, rightk,
    outq, outk, rowq, rowk, colq, colk, newq,
    halfq, halfk, wallq, wallk, pallq, pallk, o_momq, o_momk, o_preq, o_prek,
    left_lo, left_hi, right_q, spread, bq, bk, pq, pk, s_a, s_b,
    ring_recv, pair_recv, sum_recv, row_recv, col_recv, cast_recv, sems, load_sems,
):
    nf = ny * nx
    top = nz // 2
    y, x = lax.axis_index("fs_0"), lax.axis_index("fs_1")
    z, c = lax.axis_index("tp_0"), lax.axis_index("tp_1")
    fs = y * nx + x
    tp = z * 2 + c
    (ring_s, pair_s, g0q, g0k, g1q, g1k, a_s, a_r, b_s, b_r,
     h_sq, h_sk, h_rq, h_rk, m_sq, m_sk, m_rq, m_rk) = [sems.at[i] for i in range(18)]

    def row_peer(d):
        return {"fs_1": lax.rem(x + d, nx)}

    def col_peer(d):
        return {"fs_0": lax.rem(y + d, ny)}

    def plane(d):
        t = lax.rem(fs + d, nf)
        return {"fs_0": t // nx, "fs_1": lax.rem(t, nx)}

    up, down = lax.rem(z + 1, nz), lax.rem(z + nz - 1, nz)

    loads = [
        pltpu.make_async_copy(src, dst, load_sems.at[i])
        for i, (src, dst) in enumerate(
            (
                (latq, lat.at[0, c, :QF]),
                (latk, lat.at[0, c, QF:]),
                (h_wq, wq),
                (h_wk, wk),
                (cotq, cote.at[:QW]),
                (cotq.at[128:], cote.at[QW:]),
                (h_cotk, cotk),
                (h_momq, momq.at[y]),
                (h_momk, momk.at[x]),
                (h_leftq, leftq),
                (h_leftk, leftk),
                (h_rightq, rightq),
                (h_rightk, rightk),
            )
        )
    ]
    for load in loads:
        load.start()

    barrier = pltpu.get_barrier_semaphore()
    for d in ({"tp_0": up}, {"tp_0": down}, {"tp_1": 1 - c}):
        pl.semaphore_signal(barrier, inc=1, device_id=d)
    for d in range(1, nf):
        pl.semaphore_signal(barrier, inc=1, device_id=plane(d))

    select = repeat_tail()

    for load in loads[:2]:
        load.wait()
    pl.semaphore_wait(barrier, 3 + nf - 1)

    def send(src, dst, s_sem, r_sem, to):
        pltpu.make_async_remote_copy(
            src, dst, s_sem, r_sem, device_id=to, device_id_type=pl.DeviceIdType.MESH
        ).start()

    def wait(ref, sem):
        pltpu.make_async_copy(ref, ref, sem).wait()

    def part(slot, piece):
        lo, hi = PIECES[piece]
        return lat.at[slot, c, lo:hi]

    def forward(slot, to_slot, piece, to_z):
        send(
            part(slot, piece), part(to_slot, piece), ring_s,
            ring_recv.at[to_slot, piece], {"tp_0": to_z},
        )

    def share(slot, piece):
        send(part(slot, piece), part(slot, piece), pair_s, pair_recv.at[slot], {"tp_1": 1 - c})

    for p in range(len(PIECES)):
        forward(0, 1, p, up)
        forward(0, 2, p, down)
    for p in range(len(PIECES)):
        share(0, p)

    class Cast:
        def __init__(self, which, q, k):
            self.q, self.k = q, k
            self.which = which
            self.sq, self.sk, self.rq, self.rk = [cast_recv.at[which, i] for i in range(4)]

        def along_x(self, block, s_sem, r_sem):
            for d in farthest_first(nx):
                send(block, block, s_sem, r_sem, row_peer(d))

        def along_y(self, block, s_sem, r_sem):
            for d in farthest_first(ny):
                send(block, block, s_sem, r_sem, col_peer(d))

        def start(self):
            q, k = self.q.at[fs], self.k.at[fs]
            self.along_x(q, self.sq, row_recv.at[self.which, x])
            self.along_y(k, self.sk, col_recv.at[self.which, y])
            self.along_y(q, self.sq, self.rq)
            self.along_x(k, self.sk, self.rk)

        def pass_q(self, xs):
            block = self.q.at[y * nx + xs]
            wait(block, row_recv.at[self.which, xs])
            self.along_y(block, self.sq, self.rq)

        def pass_k(self, ys):
            block = self.k.at[ys * nx + x]
            wait(block, col_recv.at[self.which, ys])
            self.along_x(block, self.sk, self.rk)

        def finish(self):
            wait(self.q.at[: (ny - 1) * nx], self.rq)
            wait(self.k.at[: (nx - 1) * ny], self.rk)

        def drain(self):
            wait(self.q.at[: nf - 1], self.sq)
            wait(self.k.at[: nf - 1], self.sk)

    weights, pres = Cast(0, wallq, wallk), Cast(1, pallq, pallk)
    for load in loads[2:]:
        load.wait()
    wallq[fs] = pack_q(dot(wq[...].astype(BF16), select))
    wallk[fs] = pack_k(wk[...])
    weights.start()
    for d in farthest_first(ny):
        send(momq.at[y], momq.at[y], m_sq, m_rq, col_peer(d))
    for d in farthest_first(nx):
        send(momk.at[x], momk.at[x], m_sk, m_rk, row_peer(d))

    right_q[...] = dot(rightq[0], select).astype(BF16)
    group = min(8, nf) * QR
    split = split_halves(group)
    for at in range(0, nf * QR // group):
        cut = dot(leftq[:, at * group : (at + 1) * group], split).astype(BF16)
        left_lo[:, at * group // 2 : (at + 1) * group // 2] = cut[:, : group // 2]
        left_hi[:, at * group // 2 : (at + 1) * group // 2] = cut[:, group // 2 :]

    def partial_gradient(slot, s):
        wait(lat.at[slot, 1 - c], pair_recv.at[slot])
        lq = jnp.concatenate([lat[slot, 0, :QF, :], lat[slot, 1, :QF, :]], axis=0)
        lk = jnp.concatenate([lat[slot, 0, QF:, :], lat[slot, 1, QF:, :]], axis=0)
        outq[slot] = pack_q(dot_t(lq, cote[...]))
        outk[slot] = pack_k(dot(lk, cotk[...]))
        ys, xs = s // nx, lax.rem(s, nx)

        @pl.when(xs != x)
        def _():
            send(outq.at[slot], rowq.at[ys, x], g0q, pair_recv.at[nz + ys], {"fs_1": xs})

        @pl.when(xs == x)
        def _():
            rowq[ys, x] = outq[slot]

        @pl.when(ys != y)
        def _():
            send(outk.at[slot], rowk.at[xs, y], g0k, pair_recv.at[nz + ny + xs], {"fs_0": ys})

        @pl.when(ys == y)
        def _():
            rowk[xs, y] = outk[slot]

    def added(ref, index, n):
        total = ref[index, 0].astype(F32)
        for i in range(1, n):
            total += ref[index, i].astype(F32)
        return total

    def reduce_first(slot, s):
        ys, xs = s // nx, lax.rem(s, nx)

        @pl.when(xs == x)
        def _():
            wait(rowq.at[ys, : nx - 1], pair_recv.at[nz + ys])
            colq[ys, y] = added(rowq, ys, nx).astype(BF16)
            for d in farthest_first(ny):
                send(colq.at[ys, y], colq.at[ys, y], g1q, sum_recv.at[ys], col_peer(d))

        @pl.when(ys == y)
        def _():
            wait(rowk.at[xs, : ny - 1], pair_recv.at[nz + ny + xs])
            colk[xs, x] = added(rowk, xs, ny).astype(BF16)
            for d in farthest_first(nx):
                send(colk.at[xs, x], colk.at[xs, x], g1k, sum_recv.at[ny + xs], row_peer(d))

    def momentum(slot, s):
        ys, xs = s // nx, lax.rem(s, nx)

        @pl.when(xs == x)
        def _():
            wait(colq.at[ys, : ny - 1], sum_recv.at[ys])
            q = added(colq, ys, ny)
            tail = q[QR:]
            tail = jnp.concatenate([tail, pltpu.roll(tail, 64, 1)], axis=0)
            newq[:, :128] = beta_mom * momq[ys, :, :128] + q[:QR]
            newq[:, 128:] = beta_mom * momq[ys, :, 128:] + tail[:, :64]
            halfq[s] = pack_q(dot(newq[...].astype(BF16), select))
            for d in farthest_first(nx):
                send(halfq.at[s], halfq.at[s], h_sq, h_rq, row_peer(d))

            @pl.when(ys == y)
            def _():
                o_momq[...] = newq[...]

        @pl.when(ys == y)
        def _():
            wait(colk.at[xs, : nx - 1], sum_recv.at[ny + xs])
            k = added(colk, xs, nx)
            new_a = beta_mom * momk[xs, :, :128] + k[:KR]
            new_b = beta_mom * momk[xs, :, 128:] + k[KR:]
            halfk[s] = jnp.concatenate([new_a, new_b], axis=0).astype(BF16)
            for d in farthest_first(ny):
                send(halfk.at[s], halfk.at[s], h_sk, h_rk, col_peer(d))

            @pl.when(xs == x)
            def _():
                o_momk[:, :128] = new_a
                o_momk[:, 128:] = new_b

    def per_slot(st):
        def first(do):
            @pl.when(both(st >= 1, st <= top))
            def _():
                do(2 * st - 1, lax.rem(z + nz - st, nz))

        def second(do):
            @pl.when(both(st >= 0, st < top))
            def _():
                do(2 * st, lax.rem(z + st, nz))

        return first, second

    def ring(k, p):
        is_q = p < N_Q_PIECES
        a, b = 2 * k - 1, jnp.minimum(2 * k, nz - 1)
        last_a, last_b = (top, top - 1) if is_q else (top - 1, top)

        @pl.when(k <= last_a)
        def _():
            wait(part(a, p), ring_recv.at[a, p])

            @pl.when(k < last_a)
            def _():
                forward(a, a + 2, p, up)

            share(a, p)

        @pl.when(k <= last_b)
        def _():
            wait(part(b, p), ring_recv.at[b, p])

            @pl.when(k < last_b)
            def _():
                forward(b, jnp.minimum(b + 2, nz - 1), p, down)

            share(b, p)

    def step(k, carry):
        first, second = per_slot(k - 1)
        ring(k, 0)
        first(partial_gradient)
        ring(k, 1)
        for which in per_slot(k - 1 - REDUCE):
            which(reduce_first)
        ring(k, 2)
        second(partial_gradient)
        ring(k, 3)
        ring(k, 4)

        @pl.when(k == 3)
        def _():
            wait(momq.at[: ny - 1], m_rq)
            wait(momk.at[: nx - 1], m_rk)
            for i in range(1, nx):
                weights.pass_q(lax.rem(x + i, nx))
            for i in range(1, ny):
                weights.pass_k(lax.rem(y + i, ny))

        for which in per_slot(k - 1 - OWN):
            which(momentum)
        return carry

    lax.fori_loop(1, top + 2 + OWN, step, 0)

    outs = []

    def write(src, dst):
        outs.append(pltpu.make_async_copy(src, dst, load_sems.at[len(outs)]))
        outs[-1].start()

    row = lax.broadcasted_iota(jnp.int32, (QW, 256), 0)
    col = lax.broadcasted_iota(jnp.int32, (QW, 256), 1)
    eye = jnp.where(row == col, 1.0, 0.0).astype(BF16)

    def laid_out(q, k, to_q, to_k):
        def block(s, carry):
            tail = q[s, QR:, :]
            spread[s, :, :128] = q[s, :QR, :]
            spread[s, : QR // 2, 128:] = tail
            spread[s, QR // 2 :, 128:] = pltpu.roll(tail.astype(F32), 64, 1).astype(BF16)
            rows = pl.ds(pl.multiple_of(s * KR, KR), KR)
            to_k[rows, :128] = k[s, :KR, :]
            to_k[rows, 128:] = k[s, KR:, :]
            return carry

        lax.fori_loop(0, nf, block, 0, unroll=2)
        to_q[...] = dot_t(eye, spread[...].reshape(nf * QR, 256)).astype(BF16)

    weights.finish()
    laid_out(wallq, wallk, bq, bk)
    write(bq, to_bq)
    write(bk, to_bk)
    write(o_momq, to_momq)
    write(o_momk, to_momk)
    lane = lax.broadcasted_iota(jnp.int32, (1, 128), 1)

    def with_squares(sums, values, first):
        for i, v in enumerate(values):
            sums = jnp.where(lane == first + i, jnp.sum(v * v), sums)
        return sums

    sums = with_squares(jnp.zeros((1, 128), F32), (o_momq[...], o_momk[...]), 0)
    wait(halfq.at[: (nx - 1) * ny], h_rq)
    wait(halfk.at[: (ny - 1) * nx], h_rk)
    tail = halfq[:, QR:, :].reshape(nf * QR // 2, 128)
    left_q = jnp.concatenate(
        [
            dot(leftq[...], halfq[:, :QR, :].reshape(nf * QR, 128)),
            dot(left_lo[...], tail) + pltpu.roll(dot(left_hi[...], tail), 64, 1),
        ],
        axis=1,
    )
    left_k = jnp.concatenate(
        [
            dot(leftk[...], halfk[:, :KR, :].reshape(nf * KR, 128)),
            dot(leftk[...], halfk[:, KR:, :].reshape(nf * KR, 128)),
        ],
        axis=1,
    )
    pre_q = dot(left_q[:, :QW].astype(BF16), right_q[...])
    pre_k = dot(left_k.astype(BF16), rightk[0])
    s_a[fs] = with_squares(sums, (pre_q[:, :QW], pre_k), 2)
    for dy, dx in sorted(
        ((dy, dx) for dy in range(ny) for dx in range(nx) if dy or dx),
        key=lambda d: -min(d[0], ny - d[0]) - min(d[1], nx - d[1]),
    ):
        send(s_a.at[fs], s_a.at[fs], a_s, a_r, {**col_peer(dy), **row_peer(dx)})
    pallq[fs] = pack_q(pre_q)
    pallk[fs] = pack_k(pre_k)
    pres.start()
    o_preq[...] = pre_q[:, :QW]
    o_prek[...] = pre_k
    write(o_preq, to_preq)
    write(o_prek, to_prek)
    wait(s_a.at[: nf - 1], a_r)
    total = s_a[0]
    for i in range(1, nf):
        total += s_a[i]
    s_b[tp] = total

    def column(d):
        t = lax.rem(tp + d, 2 * nz)
        return {"tp_0": t // 2, "tp_1": lax.rem(t, 2)}

    for d in farthest_first(2 * nz):
        send(s_b.at[tp], s_b.at[tp], b_s, b_r, column(d))
    for i in range(1, nx):
        pres.pass_q(lax.rem(x + i, nx))
    for i in range(1, ny):
        pres.pass_k(lax.rem(y + i, ny))
    pres.finish()
    laid_out(pallq, pallk, pq, pk)
    write(pq, to_pq)
    write(pk, to_pk)
    wait(lat.at[: nz - 1, 0], ring_s)
    wait(lat.at[:, 0], pair_s)
    wait(outq.at[: nf - ny], g0q)
    wait(outk.at[: nf - nx], g0k)
    wait(outq.at[: ny * (ny - 1)], g1q)
    wait(outk.at[: nx * (nx - 1)], g1k)
    wait(outq.at[: ny * (nx - 1)], h_sq)
    wait(outk.at[: nx * (ny - 1)], h_sk)
    wait(momq.at[: ny - 1], m_sq)
    wait(momk.at[: nx - 1], m_sk)
    weights.drain()
    pres.drain()
    for copy in outs:
        copy.wait()
    wait(s_a.at[: nf - 1], a_s)
    wait(s_b.at[: 2 * nz - 1], b_s)
    wait(s_b.at[: 2 * nz - 1], b_r)
    total = s_b[0]
    for i in range(1, 2 * nz):
        total += s_b[i]
    o_sums[...] = total


def finish_kernel(nf, *refs):
    given, outs, held = refs[:11], refs[11:19], refs[19:30]
    upd_q, upd_k, new_wq, new_wk, copy_q, copy_k, load_sems, out_sems = refs[30:]
    to_momq, to_momk, to_updq, to_updk, to_wq, to_wk, to_cq, to_ck = outs
    loads = [
        pltpu.make_async_copy(src, dst, load_sems.at[i])
        for i, (src, dst) in enumerate(zip(given, held))
    ]
    for load in loads:
        load.start()
    sums, momq, momk, preq, prek, wq, wk, bq, pq, bk, pk = held
    started = []

    def write(src, dst):
        started.append(pltpu.make_async_copy(src, dst, out_sems.at[len(started)]))
        started[-1].start()

    loads[0].wait()
    v = sums[...]
    lane = lax.broadcasted_iota(jnp.int32, (1, 128), 1)
    scales = jnp.sqrt(v / pltpu.roll(v, 126, 1))
    scale_q, scale_k = [
        jnp.sum(jnp.where(lane == i, scales, 0.0), axis=1, keepdims=True) for i in (0, 1)
    ]
    for load in loads[1:9]:
        load.wait()
    write(momq, to_momq)
    write(momk, to_momk)

    def query(i, carry):
        rows = pl.ds(pl.multiple_of(i * 32, 32), 32)
        step = learn_rate * (scale_q * pq[rows, :].astype(F32))
        copy_q[rows, :] = (bq[rows, :].astype(F32) - step).astype(BF16)
        return carry

    lax.fori_loop(0, QW // 32, query, 0)
    write(copy_q, to_cq)
    for load in loads[9:]:
        load.wait()

    def key_value(s, carry):
        rows = pl.ds(pl.multiple_of(s * 128, 128), 128)
        step = learn_rate * (scale_k * pk[rows, :].astype(F32))
        copy_k[rows, :] = (bk[rows, :].astype(F32) - step).astype(BF16)
        return carry

    lax.fori_loop(0, nf * KR // 128, key_value, 0)
    write(copy_k, to_ck)
    upd_q[...] = scale_q * preq[...]
    upd_k[...] = scale_k * prek[...]
    new_wq[...] = wq[...] - learn_rate * upd_q[...]
    new_wk[...] = wk[...] - learn_rate * upd_k[...]
    write(upd_q, to_updq)
    write(upd_k, to_updk)
    write(new_wq, to_wq)
    write(new_wk, to_wk)
    for copy in started:
        copy.wait()


def on_device(
    ny, nx, nz,
    saved_query_latent,
    saved_key_value_latent,
    query_cot,
    kv_cot,
    query_full_weight,
    key_value_full_weight,
    query_mom,
    kv_mom,
    query_left,
    kv_left,
    query_right,
    kv_right,
):
    nf = ny * nx
    tokens = query_cot.shape[0]
    vmem = pl.BlockSpec(memory_space=pltpu.VMEM)
    shape = jax.ShapeDtypeStruct
    own_q, own_k = shape((QR, QW), F32), shape((KR, KW), F32)
    all_q, all_k = shape((QW, nf * QR), BF16), shape((nf * KR, KW), BF16)
    row = shape((1, 128), F32)
    hbm = pl.BlockSpec(memory_space=pltpu.HBM)
    block_q, block_k = [lambda *n, r=r: pltpu.VMEM((*n, r, 128), BF16) for r in (QP, KP)]
    dma = pltpu.SemaphoreType.DMA
    mom_q, mom_k, pre_q, pre_k, p_q, p_k, b_q, b_k, sums = pl.pallas_call(
        functools.partial(gather_kernel, ny, nx, nz),
        out_shape=(own_q, own_k, own_q, own_k, all_q, all_k, all_q, all_k, row),
        in_specs=[hbm] * 12,
        out_specs=(hbm,) * 8 + (vmem,),
        scratch_shapes=[
            pltpu.VMEM((nz, 2, CF, tokens), BF16),
            pltpu.VMEM((256, tokens), BF16),
            pltpu.VMEM((tokens, KW), BF16),
            pltpu.VMEM((QR, QW), F32),
            pltpu.VMEM((KR, KW), F32),
            pltpu.VMEM((ny, QR, QW), F32),
            pltpu.VMEM((nx, KR, KW), F32),
            pltpu.VMEM((QR, nf * QR), BF16),
            pltpu.VMEM((KR, nf * KR), BF16),
            pltpu.VMEM((1, QW, QW), BF16),
            pltpu.VMEM((1, KW, KW), BF16),
            block_q(nz),
            block_k(nz),
            block_q(ny, nx),
            block_k(nx, ny),
            block_q(ny, ny),
            block_k(nx, nx),
            pltpu.VMEM((QR, QW), F32),
            *(block_q(nf), block_k(nf)) * 3,
            pltpu.VMEM((QR, QW), F32),
            pltpu.VMEM((KR, KW), F32),
            pltpu.VMEM((QR, QW), F32),
            pltpu.VMEM((KR, KW), F32),
            pltpu.VMEM((QR, nf * QR // 2), BF16),
            pltpu.VMEM((QR, nf * QR // 2), BF16),
            pltpu.VMEM((QW, 256), BF16),
            pltpu.VMEM((nf, QR, 256), BF16),
            *(pltpu.VMEM((QW, nf * QR), BF16), pltpu.VMEM((nf * KR, KW), BF16)) * 2,
            pltpu.VMEM((nf, 1, 128), F32),
            pltpu.VMEM((2 * nz, 1, 128), F32),
            dma((nz, len(PIECES))),
            dma((nz + ny + nx,)),
            dma((ny + nx,)),
            dma((2, nx)),
            dma((2, ny)),
            dma((2, 4)),
            dma((18,)),
            dma((13,)),
        ],
        compiler_params=pltpu.CompilerParams(collective_id=0, has_side_effects=True),
    )(
        saved_query_latent.T, saved_key_value_latent.T, query_cot.T, kv_cot,
        query_full_weight, key_value_full_weight, query_mom, kv_mom,
        query_left, kv_left, query_right, kv_right,
    )
    given = (
        sums, mom_q, mom_k, pre_q, pre_k, query_full_weight, key_value_full_weight,
        b_q, p_q, b_k, p_k,
    )
    outs = pl.pallas_call(
        functools.partial(finish_kernel, nf),
        out_shape=(
            own_q, own_k, own_q, own_k, own_q, own_k,
            shape((QW, nf * QR), BF16), shape((nf * KR, KW), BF16),
        ),
        in_specs=[hbm] * 11,
        out_specs=(hbm,) * 8,
        scratch_shapes=[
            *(pltpu.VMEM(a.shape, a.dtype) for a in given),
            pltpu.VMEM((QR, QW), F32),
            pltpu.VMEM((KR, KW), F32),
            pltpu.VMEM((QR, QW), F32),
            pltpu.VMEM((KR, KW), F32),
            pltpu.VMEM((QW, nf * QR), BF16),
            pltpu.VMEM((nf * KR, KW), BF16),
            dma((11,)),
            dma((8,)),
        ],
    )(*given)
    return (*outs[:6], outs[6].T, outs[7])


def solution(mesh, dims=(4, 4, 16)):
    torus = Mesh(mesh.devices.reshape(*dims, 2), (*FS, *TP))
    placed = (P(FS, TP),) * 8 + (P(FS, None),) * 2 + (P(TP, None, None),) * 2
    return jax.shard_map(
        functools.partial(on_device, *dims),
        mesh=torus,
        in_specs=placed,
        out_specs=(P(FS, TP),) * 6 + (P(None, TP),) * 2,
        check_vma=False,
    )
```
